512 devices in a mesh: dp: 4 (over x), kv: 64 (over z, y), tp: 2 (over core).
Axes of the slice: x: 4, y: 8, z: 8, core: 2. Of those that a mesh axis runs over, the one named last changes fastest.
Arguments:
- tokens: bfloat16 [512, 4, 4096], P('dp', None, 'kv'), may hold values from -260 to 260
- norm_gain: bfloat16 [4096], replicated, may hold values from 0.099609375 to 1.8984375
- query_weight: bfloat16 [4096, 2048], P(None, ('tp', 'kv')), may hold values from -0.09375 to 0.09375
- key_weight: bfloat16 [4096, 2048], P(None, ('tp', 'kv')), may hold values from -0.09375 to 0.09375
- value_weight: bfloat16 [4096, 4096], P(None, ('tp', 'kv')), may hold values from -0.09375 to 0.09375
- gate_weight: bfloat16 [4096, 4096], P(None, ('tp', 'kv')), may hold values from -0.09375 to 0.09375
- out_weight: bfloat16 [4096, 4096], P('tp', 'kv'), may hold values from -0.09375 to 0.09375
- decay_rate: float32 [16], P('tp'), may hold values from 0.02 to 1
- prior_state: float32 [512, 16, 128, 256], P(('dp', 'kv'), 'tp'), may hold values from -0.6 to 0.6
- last_keys: bfloat16 [512, 4, 16, 128], P(('dp', 'kv'), None, 'tp'), may hold values from -0.5390625 to 0.5390625
- last_values: bfloat16 [512, 4, 16, 256], P(('dp', 'kv'), None, 'tp'), may hold values from -6 to 6
- accepted: int32 [512], P(('dp', 'kv')), may hold values from 0 to 4
- lengths: int32 [512], P(('dp', 'kv')), may hold values from 16 to 99999
Outputs:
- retained: bfloat16 [512, 4, 4096], P('dp', None, ('kv', 'tp'))
- new_state: float32 [512, 16, 128, 256], P(('dp', 'kv'), 'tp')
- new_keys: bfloat16 [512, 4, 16, 128], P(('dp', 'kv'), None, 'tp')
- new_values: bfloat16 [512, 4, 16, 256], P(('dp', 'kv'), None, 'tp')
The draws below stay inside these ranges and needn't reach their ends.
Inputs may be any that keep to these rules, and one draw needn't show every extreme that they name: `accepted`: how many of the last step's 4 proposals were taken.
All inputs are finite; a program needn't handle non-finite values.
Results may differ from the reference program's by a relative error of at most 0.012.
Values may be sent and summed in bfloat16 or wider, within the bound.
No kernel may reach another device: no remote copies, remote signals or barrier semaphores. Data moves between devices by JAX's collectives and lax.ppermute only.
A program may use at most 64 MiB of HBM per device.

```python
import math
import jax
import jax.numpy as jnp
from jax import lax

D = 4096
HEADS = 16
HEAD_K = 128
HEAD_V = 256
PROPOSALS = 4
SEQS = 512
N_TP = 2


def draw_tokens(key, part):
    first_key, second_key, third_key = jax.random.split(jax.random.fold_in(key, 11), 3)
    base = jax.random.normal(first_key, (SEQS, PROPOSALS, D), jnp.float32)
    base = jnp.clip(base, -6.0, 6.0)
    row_scales = jnp.exp(jax.random.uniform(second_key, (SEQS, PROPOSALS, 1), jnp.float32, 0.0, math.log(10.0)))
    ramp = jnp.exp(math.log(3.0) * jnp.arange(D, dtype=jnp.float32) / D)
    column_scales = jnp.exp(jax.random.uniform(third_key, (D,), jnp.float32, -0.35, 0.35))
    return (base * row_scales * ramp * column_scales).astype(jnp.bfloat16)


def plant(entries, stream_key, low, top_value):
    place = [jax.random.randint(jax.random.fold_in(stream_key, axis), (), 0, length) for axis, length in enumerate(entries.shape)]
    longest = entries.shape.index(max(entries.shape))
    next_to = place[:longest] + [(place[longest] + 1) % entries.shape[longest]] + place[longest + 1:]
    return entries.at[tuple(place)].set(low).at[tuple(next_to)].set(top_value)


def levels(key, shape, shards, least, top_value):
    gain, own = 1.0, jax.random.fold_in(key, 6)
    for position, parts in shards:
        draws = jnp.exp(jax.random.uniform(jax.random.fold_in(own, position), (parts,), jnp.float32, least / len(shards), top_value / len(shards)))
        gain = gain * jnp.repeat(draws, shape[position] // parts).reshape([-1 if axis == position else 1 for axis in range(len(shape))])
    return gain


def scatter_about(key, shape, scale, bound, shards=(), kind=jnp.bfloat16):
    result = jax.random.normal(key, shape, jnp.float32) * scale
    if len(shards) > 0:
        result = levels(key, shape, shards, -0.22, 0.18) * result
    return jnp.clip(result, min=-bound, max=bound).astype(kind)


def setup_inputs(seed: int = 0) -> dict:
    keys = jax.random.split(jax.random.key(seed), 14)
    tokens = draw_tokens(jax.random.fold_in(keys[13], 71), 0)
    norm_gain = jnp.clip(1.0 + 0.18 * jax.random.normal(keys[1], (D,), jnp.float32), 0.099609375, 1.8984375).astype(jnp.bfloat16)
    query_weight = scatter_about(keys[2], (D, HEADS * HEAD_K), D ** -0.5, 0.09375, ((1, 128),))
    key_weight = scatter_about(keys[3], (D, HEADS * HEAD_K), D ** -0.5, 0.09375, ((1, 128),))
    value_weight = scatter_about(keys[4], (D, HEADS * HEAD_V), D ** -0.5, 0.09375, ((1, 128),))
    gate_weight = scatter_about(keys[5], (D, HEADS * HEAD_V), D ** -0.5, 0.09375, ((1, 128),))
    out_weight = scatter_about(keys[6], (HEADS * HEAD_V, D), (HEADS * HEAD_V) ** -0.5, 0.09375, ((0, 2), (1, 64)))
    decay_rate = jnp.clip(jnp.exp(math.log(1.0) - 3.912023 * jax.random.uniform(keys[7], (HEADS,), jnp.float32) ** levels(keys[7], (HEADS,), ((0, 2),), -0.2, 0.2)), 0.02, 1.0)
    prior_state = scatter_about(keys[8], (SEQS, HEADS, HEAD_K, HEAD_V), 0.1, 0.6, ((0, 256), (1, 2)), jnp.float32)
    last_keys = scatter_about(keys[9], (SEQS, PROPOSALS, HEADS, HEAD_K), 0.09, 0.5390625, ((0, 256), (2, 2)))
    last_values = scatter_about(keys[10], (SEQS, PROPOSALS, HEADS, HEAD_V), 1.0, 6.0, ((0, 256), (2, 2)))
    accepted = plant(jax.random.randint(keys[11], (SEQS,), 0, PROPOSALS + 1), jax.random.fold_in(keys[11], 1), 0, PROPOSALS).astype(jnp.int32)
    lengths = plant(jax.random.randint(keys[12], (SEQS,), 16, 100000), jax.random.fold_in(keys[12], 1), 16, 99999).astype(jnp.int32)
    return dict(tokens=tokens, norm_gain=norm_gain, query_weight=query_weight, key_weight=key_weight, value_weight=value_weight, gate_weight=gate_weight, out_weight=out_weight, decay_rate=decay_rate, prior_state=prior_state, last_keys=last_keys, last_values=last_values, accepted=accepted, lengths=lengths)


epsilon = 1e-06

def rotate(field_in, positions):
    half_size = field_in.shape[-1] // 2
    frequency = jnp.power(10000.0, -jnp.arange(half_size, dtype=jnp.float32) / half_size)
    angles = positions.astype(jnp.float32)[:, :, None, None] * frequency
    cosine, sine_part = (jnp.cos(angles), jnp.sin(angles))
    floats = field_in.astype(jnp.float32)
    first_half, second = (floats[..., :half_size], floats[..., half_size:])
    return jnp.concatenate([first_half * cosine - second * sine_part, first_half * sine_part + second * cosine], axis=-1)

def retain(query_rot, key_rot, value_rows, prior_state, last_keys, last_values, accepted, log_decay):
    highest = lax.Precision.HIGHEST
    proposals = query_rot.shape[1]
    step_ids = jnp.arange(proposals, dtype=jnp.int32)
    taken_mask = step_ids[None, :] < accepted[:, None]
    power_exp = jnp.maximum(accepted[:, None] - 1 - step_ids[None, :], 0).astype(jnp.float32)
    weight = jnp.where(taken_mask[:, :, None], jnp.exp(log_decay[None, None, :] * power_exp[:, :, None]), 0.0)
    carried = jnp.exp(log_decay[None, :] * accepted[:, None].astype(jnp.float32))
    weighted_keys = last_keys.astype(jnp.float32) * weight[..., None]
    taken_state = carried[:, :, None, None] * prior_state + jnp.einsum('sphd,sphe->shde', weighted_keys, last_values.astype(jnp.float32), precision=highest)
    scores = jnp.einsum('sthd,smhd->shtm', query_rot.astype(jnp.float32), key_rot.astype(jnp.float32), precision=highest)
    offset = (step_ids[:, None] - step_ids[None, :]).astype(jnp.float32)
    decay_grid = jnp.where(offset[None] >= 0.0, jnp.exp(log_decay[:, None, None] * jnp.maximum(offset, 0.0)[None]), 0.0)
    inner_sum = jnp.einsum('shtm,smhe->sthe', scores * decay_grid[None], value_rows.astype(jnp.float32), precision=highest)
    query_decay = jnp.exp(log_decay[None, :] * (step_ids[:, None].astype(jnp.float32) + 1.0))
    cross_sum = jnp.einsum('sthd,shde->sthe', query_rot.astype(jnp.float32) * query_decay[None, :, :, None], taken_state, precision=highest)
    return (inner_sum + cross_sum, taken_state)

def reference(tokens, norm_gain, query_weight, key_weight, value_weight, gate_weight, out_weight, decay_rate, prior_state, last_keys, last_values, accepted, lengths):
    seq_count, proposals, width = tokens.shape
    heads = decay_rate.shape[0]
    key_size = last_keys.shape[-1]
    value_size = last_values.shape[-1]
    floats = tokens.astype(jnp.float32)
    row_stat = lax.rsqrt(lax.optimization_barrier(jnp.mean(floats * floats, axis=-1)) + epsilon)
    normed = (floats * row_stat[..., None] * norm_gain.astype(jnp.float32)).astype(jnp.bfloat16)
    normed = normed.reshape(seq_count * proposals, width)

    def project(weight, last_size):
        product = jnp.dot(normed, weight, preferred_element_type=jnp.float32).astype(jnp.bfloat16)
        return product.reshape(seq_count, proposals, heads, last_size)
    query_rows = project(query_weight, key_size)
    key_rows = project(key_weight, key_size)
    value_rows = project(value_weight, value_size)
    gate_rows = project(gate_weight, value_size)
    positions = (lengths + accepted)[:, None] + jnp.arange(proposals, dtype=jnp.int32)[None, :]
    query_rot = rotate(query_rows, positions).astype(jnp.bfloat16)
    key_rot = (rotate(key_rows, positions) * key_size ** (-0.5)).astype(jnp.bfloat16)
    heads_out, taken_state = retain(query_rot, key_rot, value_rows, prior_state, last_keys, last_values, accepted, -decay_rate)
    head_norm = heads_out * lax.rsqrt(lax.optimization_barrier(jnp.mean(heads_out * heads_out, axis=-1, keepdims=True)) + epsilon)
    gated = (jax.nn.silu(gate_rows.astype(jnp.float32)) * head_norm).astype(jnp.bfloat16)
    gated = gated.reshape(seq_count * proposals, heads * value_size)
    group_rows = heads * value_size // N_TP
    summed = jnp.zeros((seq_count * proposals, width), jnp.float32)
    for block in range(N_TP):
        partial_sum = jnp.dot(gated[:, block * group_rows:(block + 1) * group_rows], out_weight[block * group_rows:(block + 1) * group_rows], preferred_element_type=jnp.float32)
        rounded = lax.optimization_barrier(partial_sum.astype(jnp.bfloat16))
        summed = summed + rounded.astype(jnp.float32)
    retained = summed.astype(jnp.bfloat16).reshape(seq_count, proposals, width)
    return (retained, taken_state, key_rot, value_rows)
```

```python
import jax
import jax.numpy as jnp
from jax import lax
from jax.experimental import pallas as pl
from jax.experimental.pallas import tpu as pltpu
from jax.sharding import Mesh
from jax.sharding import PartitionSpec as P

KV = ("kv_0", "kv_1")
TP_KV = ("tp", "kv_0", "kv_1")
DP_KV = ("dp", "kv_0", "kv_1")
KV_TP = ("kv_0", "kv_1", "tp")


epsilon = 1e-06
FLOAT = jnp.float32
HALF = jnp.bfloat16


def moved(value, axis, target):
    size = lax.axis_size(axis)
    return lax.ppermute(value, axis, [(i, target(i) % size) for i in range(size)])


def scattered(blocks, axes):
    return lax.all_to_all(blocks, axes, 0, 0, tiled=True)


def rotate(field_in, positions):
    half_size = field_in.shape[-1] // 2
    frequency = jnp.power(10000.0, -jnp.arange(half_size, dtype=FLOAT) / half_size)
    angles = positions.astype(FLOAT)[:, :, None, None] * frequency
    cosine, sine_part = (jnp.cos(angles), jnp.sin(angles))
    floats = field_in.astype(FLOAT)
    first_half, second = (floats[..., :half_size], floats[..., half_size:])
    return jnp.concatenate(
        [first_half * cosine - second * sine_part, first_half * sine_part + second * cosine],
        axis=-1,
    )


def next_state(prior_state, last_keys, last_values, accepted, log_decay):
    highest = lax.Precision.HIGHEST
    step_ids = jnp.arange(last_keys.shape[1], dtype=jnp.int32)
    taken_mask = step_ids[None, :] < accepted[:, None]
    power_exp = jnp.maximum(accepted[:, None] - 1 - step_ids[None, :], 0).astype(FLOAT)
    weight = jnp.where(
        taken_mask[:, :, None], jnp.exp(log_decay[None, None, :] * power_exp[:, :, None]), 0.0
    )
    carried = jnp.exp(log_decay[None, :] * accepted[:, None].astype(FLOAT))
    weighted_keys = last_keys.astype(FLOAT) * weight[..., None]
    return carried[:, :, None, None] * prior_state + jnp.einsum(
        "sphd,sphe->shde", weighted_keys, last_values.astype(FLOAT), precision=highest
    )


def retain(query_rot, key_rot, value_rows, taken_state, log_decay):
    highest = lax.Precision.HIGHEST
    step_ids = jnp.arange(query_rot.shape[1], dtype=jnp.int32)
    scores = jnp.einsum(
        "sthd,smhd->shtm", query_rot.astype(FLOAT), key_rot.astype(FLOAT), precision=highest
    )
    offset = (step_ids[:, None] - step_ids[None, :]).astype(FLOAT)
    decay_grid = jnp.where(
        offset[None] >= 0.0, jnp.exp(log_decay[:, None, None] * jnp.maximum(offset, 0.0)[None]), 0.0
    )
    inner_sum = jnp.einsum(
        "shtm,smhe->sthe", scores * decay_grid[None], value_rows.astype(FLOAT), precision=highest
    )
    query_decay = jnp.exp(log_decay[None, :] * (step_ids[:, None].astype(FLOAT) + 1.0))
    cross_sum = jnp.einsum(
        "sthd,shde->sthe",
        query_rot.astype(FLOAT) * query_decay[None, :, :, None],
        taken_state,
        precision=highest,
    )
    return inner_sum + cross_sum


def project_kernel(place, rows, gain, w_own, w_near, w_pair, w_far, out, weights):
    core, parity = place[0], place[1]
    width = gain.shape[1]
    key_cols = w_own.shape[0] // 6
    span = 2 * w_own.shape[0]
    scale = gain[...].astype(FLOAT)
    for source, same_core, same_row in (
        (w_own, True, True),
        (w_near, True, False),
        (w_pair, False, True),
        (w_far, False, False),
    ):
        head_group = core if same_core else 1 - core
        later = parity if same_row else 1 - parity
        first = 0
        for size in (key_cols, key_cols, 2 * key_cols, 2 * key_cols):
            start = pl.multiple_of(head_group * span + 2 * first + later * size, 16)
            picked = source[first : first + size, :].astype(FLOAT) * scale
            weights[pl.ds(start, size), :] = picked.astype(HALF)
            first += size
    values = rows[...]
    floats = values.astype(FLOAT)
    squares = jnp.sum(floats * floats, axis=0, keepdims=True)
    row_scale = lax.rsqrt(squares / width + epsilon)
    product = jnp.dot(weights[...], values, preferred_element_type=FLOAT) * row_scale
    for head_group in range(2):
        part = product[head_group * span : (head_group + 1) * span]
        out[head_group] = part.T.astype(HALF)


def project(place, rows, gain, w_own, w_near, w_pair, w_far):
    span = 2 * w_own.shape[0]
    vmem = pl.BlockSpec(memory_space=pltpu.VMEM)
    return pl.pallas_call(
        project_kernel,
        in_specs=[pl.BlockSpec(memory_space=pltpu.SMEM)] + [vmem] * 6,
        out_specs=vmem,
        out_shape=jax.ShapeDtypeStruct((2, rows.shape[1], span), HALF),
        scratch_shapes=[pltpu.VMEM((2 * span, rows.shape[0]), HALF)],
        name="project",
    )(place, rows, gain, w_own, w_near, w_pair, w_far)


def output_kernel(place, rows, *refs):
    blocks, out, weights, product = refs[:-3], refs[-3], refs[-2], refs[-1]
    z, ring = place[0], 8
    cols = blocks[0].shape[0]
    quarter = cols // 2
    for shift, block in zip((0, -1, 1, -2, 2, -3, 3), blocks):
        start = pl.multiple_of(lax.rem(z + shift + ring, ring) * cols, cols)
        weights[pl.ds(start, cols), :] = block[...]
    opposite = lax.rem(z + 4, ring) * cols
    for side, block in enumerate(blocks[7:]):
        start = pl.multiple_of(opposite + side * quarter, quarter)
        weights[pl.ds(start, quarter), :] = block[...]
    total = lax.dot_general(
        rows[...], weights[...], (((1,), (1,)), ((), ())), preferred_element_type=FLOAT
    )
    groups, row_count, lanes = product.shape
    for group in range(groups):
        product[group] = total[:, group * lanes : (group + 1) * lanes]
    proposals = 4
    seqs = row_count // proposals
    for group in range(groups):
        parts = [product[group, pl.ds(p, seqs, stride=proposals), :] for p in range(proposals)]
        for block in range(lanes // quarter):
            pieces = [part[:, block * quarter : (block + 1) * quarter] for part in parts]
            joined = jnp.concatenate(pieces, axis=1)
            out[group * (lanes // quarter) + block] = joined.astype(HALF)


def output_product(place, rows, blocks):
    vmem = pl.BlockSpec(memory_space=pltpu.VMEM)
    cols, depth = blocks[0].shape
    quarter = cols // 2
    row_count = rows.shape[0]
    return pl.pallas_call(
        output_kernel,
        in_specs=[pl.BlockSpec(memory_space=pltpu.SMEM)] + [vmem] * (1 + len(blocks)),
        out_specs=vmem,
        out_shape=jax.ShapeDtypeStruct((16, row_count // 4, 4 * quarter), HALF),
        scratch_shapes=[
            pltpu.VMEM((8 * cols, depth), HALF),
            pltpu.VMEM((8 * cols // 128, row_count, 128), FLOAT),
        ],
        name="output",
    )(place, rows, *blocks)


def shards(
    tokens,
    norm_gain,
    query_weight,
    key_weight,
    value_weight,
    gate_weight,
    out_weight,
    decay_rate,
    prior_state,
    last_keys,
    last_values,
    accepted,
    lengths,
):
    owned_seqs, proposals, own_width = tokens.shape
    local_seqs, heads_here, key_size, value_size = prior_state.shape
    width = norm_gain.shape[0]
    core = lax.axis_index("tp")
    y_index = lax.axis_index("kv_1")
    z_index = lax.axis_index("kv_0")

    turned = tokens.transpose(1, 2, 0)
    mine = lax.dynamic_slice_in_dim(turned, 2 * core, 2, 0)
    copies = jnp.broadcast_to(mine[None], (32, 2, own_width, owned_seqs))
    copies = copies.reshape(64, own_width, owned_seqs)
    arrived = scattered(copies, KV)

    w_own = jnp.concatenate(
        [query_weight.T, key_weight.T, value_weight.T, gate_weight.T], axis=0
    )
    w_near = moved(w_own, "kv_1", lambda i: i ^ 1)
    w_pair = moved(w_own, "tp", lambda i: i ^ 1)
    w_far = moved(w_near, "tp", lambda i: i ^ 1)

    o_own = out_weight.T
    up, down = [o_own], [o_own]
    for _ in range(3):
        up.append(moved(up[-1], "kv_0", lambda i: i + 1))
        down.append(moved(down[-1], "kv_0", lambda i: i - 1))
    part = o_own.shape[0] // 2
    last_up = moved(up[-1][:part], "kv_0", lambda i: i + 1)
    last_down = moved(down[-1][part:], "kv_0", lambda i: i - 1)
    out_blocks = [o_own, up[1], down[1], up[2], down[2], up[3], down[3], last_up, last_down]

    log_decay = -decay_rate
    taken_state = next_state(prior_state, last_keys, last_values, accepted, log_decay)

    place = jnp.stack([core, y_index & 1]).astype(jnp.int32)
    columns = project(
        place,
        arrived.reshape(width, owned_seqs),
        norm_gain.reshape(1, width),
        w_own,
        w_near,
        w_pair,
        w_far,
    )
    span = columns.shape[-1]
    columns = columns.reshape(2, 64, local_seqs, span).transpose(1, 0, 2, 3)
    columns = scattered(columns.reshape(128, local_seqs, span), KV_TP)
    pieces = columns.reshape(8, 4, 2, 2, local_seqs, span)

    def role_rows(first, last, size):
        picked = pieces[..., first:last].transpose(4, 3, 2, 0, 1, 5)
        return picked.reshape(local_seqs, proposals, heads_here, size)

    sixth = span // 6
    query_rows = role_rows(0, sixth, key_size)
    key_rows = role_rows(sixth, 2 * sixth, key_size)
    value_rows = role_rows(2 * sixth, 4 * sixth, value_size)
    gate_rows = role_rows(4 * sixth, 6 * sixth, value_size)
    positions = (lengths + accepted)[:, None] + jnp.arange(proposals, dtype=jnp.int32)[None, :]
    query_rot = rotate(query_rows, positions).astype(HALF)
    key_rot = (rotate(key_rows, positions) * key_size ** (-0.5)).astype(HALF)
    heads_out = retain(query_rot, key_rot, value_rows, taken_state, log_decay)
    head_norm = heads_out * lax.rsqrt(
        jnp.mean(heads_out * heads_out, axis=-1, keepdims=True) + epsilon
    )
    gated = (jax.nn.silu(gate_rows.astype(FLOAT)) * head_norm).astype(HALF)
    depth = heads_here * value_size
    gated = gated.reshape(1, local_seqs * proposals, depth)
    gathered = scattered(jnp.broadcast_to(gated, (8, local_seqs * proposals, depth)), "kv_1")
    z_place = z_index.reshape(1).astype(jnp.int32)
    partial_out = output_product(
        z_place, gathered.reshape(8 * local_seqs * proposals, depth), out_blocks
    )
    terms = scattered(partial_out, ("kv_0", "tp"))
    terms = terms.reshape(8, 2, *terms.shape[1:]).astype(FLOAT)
    retained = (terms[:, 0] + terms[:, 1]).astype(HALF)
    retained = retained.reshape(owned_seqs, proposals, -1)
    return (retained, taken_state, key_rot, value_rows)


def solution(mesh):
    finer = Mesh(
        mesh.devices.reshape(mesh.shape["dp"], 8, 8, mesh.shape["tp"]), ("dp", "kv_0", "kv_1", "tp")
    )
    return jax.shard_map(
        shards,
        mesh=finer,
        in_specs=(
            P("dp", None, KV),
            P(),
            P(None, TP_KV),
            P(None, TP_KV),
            P(None, TP_KV),
            P(None, TP_KV),
            P("tp", KV),
            P("tp"),
            P(DP_KV, "tp", None, None),
            P(DP_KV, None, "tp", None),
            P(DP_KV, None, "tp", None),
            P(DP_KV),
            P(DP_KV),
        ),
        out_specs=(
            P("dp", None, KV_TP),
            P(DP_KV, "tp", None, None),
            P(DP_KV, None, "tp", None),
            P(DP_KV, None, "tp", None),
        ),
        check_vma=False,
    )
```

```python
import jax
import jax.numpy as jnp
from jax import lax
from jax.experimental import pallas as pl
from jax.experimental.pallas import tpu as pltpu
from jax.sharding import Mesh
from jax.sharding import PartitionSpec as P


KV = ("far_z", "near_z", "y")
TP_KV = ("tp", *KV)
DP_KV = ("dp", *KV)
KV_TP = (*KV, "tp")


epsilon = 1e-06
FLOAT = jnp.float32
HALF = jnp.bfloat16


def moved(value, axis, target):
    size = lax.axis_size(axis)
    return lax.ppermute(value, axis, [(i, target(i) % size) for i in range(size)])


def scattered(blocks, axes):
    return lax.all_to_all(blocks, axes, 0, 0, tiled=True)


def rotate(field_in, positions):
    half_size = field_in.shape[-1] // 2
    frequency = jnp.power(10000.0, -jnp.arange(half_size, dtype=FLOAT) / half_size)
    angles = positions.astype(FLOAT)[:, :, None, None] * frequency
    cosine, sine_part = (jnp.cos(angles), jnp.sin(angles))
    floats = field_in.astype(FLOAT)
    first_half, second = (floats[..., :half_size], floats[..., half_size:])
    return jnp.concatenate(
        [first_half * cosine - second * sine_part, first_half * sine_part + second * cosine],
        axis=-1,
    )


def next_state(prior_state, last_keys, last_values, accepted, log_decay):
    highest = lax.Precision.HIGHEST
    step_ids = jnp.arange(last_keys.shape[1], dtype=jnp.int32)
    taken_mask = step_ids[None, :] < accepted[:, None]
    power_exp = jnp.maximum(accepted[:, None] - 1 - step_ids[None, :], 0).astype(FLOAT)
    weight = jnp.where(
        taken_mask[:, :, None], jnp.exp(log_decay[None, None, :] * power_exp[:, :, None]), 0.0
    )
    carried = jnp.exp(log_decay[None, :] * accepted[:, None].astype(FLOAT))
    weighted_keys = last_keys.astype(FLOAT) * weight[..., None]
    return carried[:, :, None, None] * prior_state + jnp.einsum(
        "sphd,sphe->shde", weighted_keys, last_values.astype(FLOAT), precision=highest
    )


def retain(query_rot, key_rot, value_rows, taken_state, log_decay):
    highest = lax.Precision.HIGHEST
    step_ids = jnp.arange(query_rot.shape[1], dtype=jnp.int32)
    scores = jnp.einsum(
        "sthd,smhd->shtm", query_rot.astype(FLOAT), key_rot.astype(FLOAT), precision=highest
    )
    offset = (step_ids[:, None] - step_ids[None, :]).astype(FLOAT)
    decay_grid = jnp.where(
        offset[None] >= 0.0, jnp.exp(log_decay[:, None, None] * jnp.maximum(offset, 0.0)[None]), 0.0
    )
    inner_sum = jnp.einsum(
        "shtm,smhe->sthe", scores * decay_grid[None], value_rows.astype(FLOAT), precision=highest
    )
    query_decay = jnp.exp(log_decay[None, :] * (step_ids[:, None].astype(FLOAT) + 1.0))
    cross_sum = jnp.einsum(
        "sthd,shde->sthe",
        query_rot.astype(FLOAT) * query_decay[None, :, :, None],
        taken_state,
        precision=highest,
    )
    return inner_sum + cross_sum


def arrange_kernel(place, w_own, w_near, w_pair, w_far, weights):
    core, parity = place[0], place[1]
    key_cols = w_own.shape[0] // 6
    span = 2 * w_own.shape[0]
    for source, same_core, same_row in (
        (w_own, True, True),
        (w_near, True, False),
        (w_pair, False, True),
        (w_far, False, False),
    ):
        head_group = core if same_core else 1 - core
        later = parity if same_row else 1 - parity
        first = 0
        for size in (key_cols, key_cols, 2 * key_cols, 2 * key_cols):
            start = pl.multiple_of(head_group * span + 2 * first + later * size, 16)
            weights[pl.ds(start, size), :] = source[first : first + size, :]
            first += size


def arrange(place, sources):
    cols, width = sources[0].shape
    vmem = pl.BlockSpec(memory_space=pltpu.VMEM)
    return pl.pallas_call(
        arrange_kernel,
        in_specs=[pl.BlockSpec(memory_space=pltpu.SMEM)] + [vmem] * 4,
        out_specs=vmem,
        out_shape=jax.ShapeDtypeStruct((4 * cols, width), HALF),
        name="arrange",
    )(place, *sources)


def project_kernel(rows, gain, weights, out):
    width = rows.shape[0]
    span = weights.shape[0] // 2
    floats = rows[...].astype(FLOAT)
    squares = jnp.sum(floats * floats, axis=0, keepdims=True)
    row_scale = lax.rsqrt(squares / width + epsilon)
    normed = (floats * row_scale * gain[...].astype(FLOAT)).astype(HALF)
    product = jnp.dot(weights[...], normed, preferred_element_type=FLOAT)
    seqs = out.shape[2]
    for head_group in range(2):
        part = product[head_group * span : (head_group + 1) * span].T
        out[:, head_group] = part.reshape(-1, seqs, span).astype(HALF)


def project(rows, gain, weights):
    vmem = pl.BlockSpec(memory_space=pltpu.VMEM)
    return pl.pallas_call(
        project_kernel,
        in_specs=[vmem] * 3,
        out_specs=vmem,
        out_shape=jax.ShapeDtypeStruct((64, 2, 2, weights.shape[0] // 2), HALF),
        name="project",
    )(rows, gain, weights)


def output_kernel(place, rows, *refs):
    blocks, out, weights, product = refs[:-3], refs[-3], refs[-2], refs[-1]
    here, ring = place[0], 4
    cols = blocks[0].shape[0]
    quarter = cols // 2
    for turn, block in zip((0, 1, 3, 2), blocks):
        start = pl.multiple_of(lax.rem(here + ring - turn, ring) * cols, cols)
        weights[pl.ds(start, cols), :] = block[...]
    total = lax.dot_general(
        rows[...], weights[...], (((1,), (1,)), ((), ())), preferred_element_type=FLOAT
    )
    groups, row_count, lanes = product.shape
    for group in range(groups):
        product[group] = total[:, group * lanes : (group + 1) * lanes]
    proposals = 4
    seqs = row_count // proposals
    for group in range(groups):
        parts = [product[group, pl.ds(p, seqs, stride=proposals), :] for p in range(proposals)]
        for block in range(lanes // quarter):
            pieces = [part[:, block * quarter : (block + 1) * quarter] for part in parts]
            joined = jnp.concatenate(pieces, axis=1)
            out[group * (lanes // quarter) + block] = joined.astype(HALF)


def output_product(place, rows, blocks):
    vmem = pl.BlockSpec(memory_space=pltpu.VMEM)
    cols, depth = blocks[0].shape
    quarter = cols // 2
    row_count = rows.shape[0]
    return pl.pallas_call(
        output_kernel,
        in_specs=[pl.BlockSpec(memory_space=pltpu.SMEM)] + [vmem] * (1 + len(blocks)),
        out_specs=vmem,
        out_shape=jax.ShapeDtypeStruct((8, row_count // 4, 4 * quarter), HALF),
        scratch_shapes=[
            pltpu.VMEM((4 * cols, depth), HALF),
            pltpu.VMEM((4 * cols // 128, row_count, 128), FLOAT),
        ],
        name="output",
    )(place, rows, *blocks)


def shards(
    tokens,
    norm_gain,
    query_weight,
    key_weight,
    value_weight,
    gate_weight,
    out_weight,
    decay_rate,
    prior_state,
    last_keys,
    last_values,
    accepted,
    lengths,
):
    owned_seqs, proposals, own_width = tokens.shape
    local_seqs, heads_here, key_size, value_size = prior_state.shape
    width = norm_gain.shape[0]
    core = lax.axis_index("tp")
    y_index = lax.axis_index("y")
    far_index = lax.axis_index("far_z")

    turned = tokens.transpose(1, 2, 0)
    mine = lax.dynamic_slice_in_dim(turned, 2 * core, 2, 0)
    copies = jnp.broadcast_to(mine[None], (32, 2, own_width, owned_seqs))
    copies = copies.reshape(64, own_width, owned_seqs)
    arrived = scattered(copies, KV)

    w_own = jnp.concatenate(
        [query_weight.T, key_weight.T, value_weight.T, gate_weight.T], axis=0
    )
    w_near = moved(w_own, "y", lambda i: i ^ 1)
    w_pair = moved(w_own, "tp", lambda i: i ^ 1)
    w_far = moved(w_near, "tp", lambda i: i ^ 1)

    o_own = out_weight.T
    out_blocks = [o_own] + [
        moved(o_own, "far_z", lambda i, turn=turn: i + turn) for turn in (1, 3, 2)
    ]

    log_decay = -decay_rate
    taken_state = next_state(prior_state, last_keys, last_values, accepted, log_decay)

    place = jnp.stack([core, y_index & 1]).astype(jnp.int32)
    weights = arrange(place, (w_own, w_near, w_pair, w_far))
    gain = jnp.broadcast_to(norm_gain[:, None], (width, owned_seqs))
    columns = project(arrived.reshape(width, owned_seqs), gain, weights)
    span = columns.shape[-1]
    columns = scattered(columns.reshape(128, local_seqs, span), KV_TP)
    pieces = columns.reshape(8, 4, 2, 2, local_seqs, span)

    def role_rows(first, last, size):
        picked = pieces[..., first:last].transpose(4, 3, 2, 0, 1, 5)
        return picked.reshape(local_seqs, proposals, heads_here, size)

    sixth = span // 6
    query_rows = role_rows(0, sixth, key_size)
    key_rows = role_rows(sixth, 2 * sixth, key_size)
    value_rows = role_rows(2 * sixth, 4 * sixth, value_size)
    gate_rows = role_rows(4 * sixth, 6 * sixth, value_size)
    positions = (lengths + accepted)[:, None] + jnp.arange(proposals, dtype=jnp.int32)[None, :]
    query_rot = rotate(query_rows, positions).astype(HALF)
    key_rot = (rotate(key_rows, positions) * key_size ** (-0.5)).astype(HALF)
    heads_out = retain(query_rot, key_rot, value_rows, taken_state, log_decay)
    head_norm = heads_out * lax.rsqrt(
        jnp.mean(heads_out * heads_out, axis=-1, keepdims=True) + epsilon
    )
    gated = (jax.nn.silu(gate_rows.astype(FLOAT)) * head_norm).astype(HALF)
    depth = heads_here * value_size
    gated = gated.reshape(1, local_seqs * proposals, depth)
    gated = jnp.broadcast_to(gated, (16, local_seqs * proposals, depth))
    gathered = scattered(gated, ("near_z", "y"))
    far_place = far_index.reshape(1).astype(jnp.int32)
    partial_out = output_product(
        far_place, gathered.reshape(16 * local_seqs * proposals, depth), out_blocks
    )
    terms = scattered(partial_out, ("far_z", "tp"))
    terms = terms.reshape(4, 2, *terms.shape[1:]).astype(FLOAT)
    retained = (terms[:, 0] + terms[:, 1]).astype(HALF)
    retained = retained.reshape(owned_seqs, proposals, -1)
    return (retained, taken_state, key_rot, value_rows)


def solution(mesh):
    finer = Mesh(
        mesh.devices.reshape(mesh.shape["dp"], 4, 2, 8, mesh.shape["tp"]), ("dp", *KV, "tp")
    )
    return jax.shard_map(
        shards,
        mesh=finer,
        in_specs=(
            P("dp", None, KV),
            P(),
            P(None, TP_KV),
            P(None, TP_KV),
            P(None, TP_KV),
            P(None, TP_KV),
            P("tp", KV),
            P("tp"),
            P(DP_KV, "tp", None, None),
            P(DP_KV, None, "tp", None),
            P(DP_KV, None, "tp", None),
            P(DP_KV),
            P(DP_KV),
        ),
        out_specs=(
            P("dp", None, KV_TP),
            P(DP_KV, "tp", None, None),
            P(DP_KV, None, "tp", None),
            P(DP_KV, None, "tp", None),
        ),
        check_vma=False,
    )
```

```python
import jax
import jax.numpy as jnp
from jax import lax
from jax.experimental import pallas as pl
from jax.experimental.pallas import tpu as pltpu
from jax.sharding import Mesh
from jax.sharding import PartitionSpec as P


KV = ("far_z", "near_z", "y")
TP_KV = ("tp", *KV)
DP_KV = ("dp", *KV)
KV_TP = (*KV, "tp")


epsilon = 1e-06
FLOAT = jnp.float32
HALF = jnp.bfloat16


def moved(value, axis, target):
    size = lax.axis_size(axis)
    return lax.ppermute(value, axis, [(i, target(i) % size) for i in range(size)])


def scattered(blocks, axes):
    return lax.all_to_all(blocks, axes, 0, 0, tiled=True)


def near(value):
    return pltpu.with_memory_space_constraint(value, pltpu.VMEM)


def rotate(field_in, positions):
    half_size = field_in.shape[-1] // 2
    frequency = jnp.power(10000.0, -jnp.arange(half_size, dtype=FLOAT) / half_size)
    angles = positions.astype(FLOAT)[:, :, None, None] * frequency
    cosine, sine_part = (jnp.cos(angles), jnp.sin(angles))
    floats = field_in.astype(FLOAT)
    first_half, second = (floats[..., :half_size], floats[..., half_size:])
    return jnp.concatenate(
        [first_half * cosine - second * sine_part, first_half * sine_part + second * cosine],
        axis=-1,
    )


def next_state(prior_state, last_keys, last_values, accepted, log_decay):
    highest = lax.Precision.HIGHEST
    step_ids = jnp.arange(last_keys.shape[1], dtype=jnp.int32)
    taken_mask = step_ids[None, :] < accepted[:, None]
    power_exp = jnp.maximum(accepted[:, None] - 1 - step_ids[None, :], 0).astype(FLOAT)
    weight = jnp.where(
        taken_mask[:, :, None], jnp.exp(log_decay[None, None, :] * power_exp[:, :, None]), 0.0
    )
    carried = jnp.exp(log_decay[None, :] * accepted[:, None].astype(FLOAT))
    weighted_keys = last_keys.astype(FLOAT) * weight[..., None]
    return carried[:, :, None, None] * prior_state + jnp.einsum(
        "sphd,sphe->shde", weighted_keys, last_values.astype(FLOAT), precision=highest
    )


def retain(query_rot, key_rot, value_rows, taken_state, log_decay):
    highest = lax.Precision.HIGHEST
    step_ids = jnp.arange(query_rot.shape[1], dtype=jnp.int32)
    scores = jnp.einsum(
        "sthd,smhd->shtm", query_rot.astype(FLOAT), key_rot.astype(FLOAT), precision=highest
    )
    offset = (step_ids[:, None] - step_ids[None, :]).astype(FLOAT)
    decay_grid = jnp.where(
        offset[None] >= 0.0, jnp.exp(log_decay[:, None, None] * jnp.maximum(offset, 0.0)[None]), 0.0
    )
    inner_sum = jnp.einsum(
        "shtm,smhe->sthe", scores * decay_grid[None], value_rows.astype(FLOAT), precision=highest
    )
    query_decay = jnp.exp(log_decay[None, :] * (step_ids[:, None].astype(FLOAT) + 1.0))
    cross_sum = jnp.einsum(
        "sthd,shde->sthe",
        query_rot.astype(FLOAT) * query_decay[None, :, :, None],
        taken_state,
        precision=highest,
    )
    return inner_sum + cross_sum


def arrange_kernel(place, gain, w_own, w_near, w_pair, w_far, weights, columns):
    core, parity = place[0], place[1]
    key_cols = w_own.shape[0] // 6
    span = 2 * w_own.shape[0]
    for source, same_core, same_row in (
        (w_own, True, True),
        (w_near, True, False),
        (w_pair, False, True),
        (w_far, False, False),
    ):
        head_group = core if same_core else 1 - core
        later = parity if same_row else 1 - parity
        first = 0
        for size in (key_cols, key_cols, 2 * key_cols, 2 * key_cols):
            start = pl.multiple_of(head_group * span + 2 * first + later * size, 16)
            weights[pl.ds(start, size), :] = source[first : first + size, :]
            first += size
    side = gain.shape[1]
    floats = gain[...].astype(FLOAT)
    for row in range(gain.shape[0]):
        square = jnp.broadcast_to(floats[row : row + 1], (side, side)).T
        columns[row * side : (row + 1) * side, :] = square.astype(HALF)


def arrange(place, gain, sources):
    cols, width = sources[0].shape
    vmem = pl.BlockSpec(memory_space=pltpu.VMEM)
    side = gain.shape[1]
    return pl.pallas_call(
        arrange_kernel,
        in_specs=[pl.BlockSpec(memory_space=pltpu.SMEM)] + [vmem] * 5,
        out_specs=(vmem, vmem),
        out_shape=(
            pltpu.HBM((4 * cols, width), HALF),
            pltpu.VMEM((width, side), HALF),
        ),
        name="arrange",
        compiler_params=pltpu.CompilerParams(vmem_limit_bytes=16 << 20),
    )(place, gain, *sources)


def project_kernel(rows, gain, far_weights, out, weights, arrival):
    fetch = pltpu.make_async_copy(far_weights, weights, arrival)
    fetch.start()
    width = rows.shape[0]
    span = weights.shape[0] // 2
    floats = rows[...].astype(FLOAT)
    squares = jnp.sum(floats * floats, axis=0, keepdims=True)
    row_scale = lax.rsqrt(squares / width + epsilon)
    normed = (floats * row_scale * gain[...].astype(FLOAT)).astype(HALF)
    fetch.wait()
    product = jnp.dot(weights[...], normed, preferred_element_type=FLOAT)
    seqs = out.shape[2]
    for head_group in range(2):
        part = product[head_group * span : (head_group + 1) * span].T
        out[:, head_group] = part.reshape(-1, seqs, span).astype(HALF)


def project(rows, gain, weights):
    vmem = pl.BlockSpec(memory_space=pltpu.VMEM)
    return pl.pallas_call(
        project_kernel,
        in_specs=[vmem, vmem, pl.BlockSpec(memory_space=pltpu.HBM)],
        out_specs=vmem,
        out_shape=pltpu.VMEM((64, 2, 2, weights.shape[0] // 2), HALF),
        scratch_shapes=[pltpu.VMEM(weights.shape, HALF), pltpu.SemaphoreType.DMA],
        name="project",
        compiler_params=pltpu.CompilerParams(vmem_limit_bytes=24 << 20),
    )(near(rows), near(gain), pltpu.with_memory_space_constraint(weights, pltpu.HBM))


def output_kernel(place, rows, *refs):
    blocks, out, weights, product = refs[:-3], refs[-3], refs[-2], refs[-1]
    here, ring = place[0], 4
    cols = blocks[0].shape[0]
    quarter = cols // 2
    stride = 2 * place[1] - 1
    for turn, block in zip((0, stride, -stride, 2), blocks):
        start = pl.multiple_of(lax.rem(here + ring + turn, ring) * cols, cols)
        weights[pl.ds(start, cols), :] = block[...]
    total = lax.dot_general(
        rows[...], weights[...], (((1,), (1,)), ((), ())), preferred_element_type=FLOAT
    )
    groups, row_count, lanes = product.shape
    for group in range(groups):
        product[group] = total[:, group * lanes : (group + 1) * lanes]
    proposals = 4
    seqs = row_count // proposals
    for group in range(groups):
        parts = [product[group, pl.ds(p, seqs, stride=proposals), :] for p in range(proposals)]
        for block in range(lanes // quarter):
            pieces = [part[:, block * quarter : (block + 1) * quarter] for part in parts]
            joined = jnp.concatenate(pieces, axis=1)
            out[group * (lanes // quarter) + block] = joined.astype(HALF)


def output_product(place, rows, blocks):
    vmem = pl.BlockSpec(memory_space=pltpu.VMEM)
    cols, depth = blocks[0].shape
    quarter = cols // 2
    row_count = rows.shape[0]
    return pl.pallas_call(
        output_kernel,
        in_specs=[pl.BlockSpec(memory_space=pltpu.SMEM)] + [vmem] * (1 + len(blocks)),
        out_specs=vmem,
        out_shape=pltpu.VMEM((8, row_count // 4, 4 * quarter), HALF),
        scratch_shapes=[
            pltpu.VMEM((4 * cols, depth), HALF),
            pltpu.VMEM((4 * cols // 128, row_count, 128), FLOAT),
        ],
        name="output",
        compiler_params=pltpu.CompilerParams(vmem_limit_bytes=16 << 20),
    )(place, near(rows), *blocks)


def shards(
    tokens,
    norm_gain,
    query_weight,
    key_weight,
    value_weight,
    gate_weight,
    out_weight,
    decay_rate,
    prior_state,
    last_keys,
    last_values,
    accepted,
    lengths,
):
    owned_seqs, proposals, own_width = tokens.shape
    local_seqs, heads_here, key_size, value_size = prior_state.shape
    width = norm_gain.shape[0]
    core = lax.axis_index("tp")
    y_index = lax.axis_index("y")
    far_index = lax.axis_index("far_z")

    turned = tokens.transpose(1, 2, 0)
    mine = lax.dynamic_slice_in_dim(turned, 2 * core, 2, 0)
    copies = jnp.broadcast_to(mine[None], (32, 2, own_width, owned_seqs))
    copies = copies.reshape(64, own_width, owned_seqs)
    arrived = scattered(copies, KV)

    w_own = jnp.concatenate(
        [query_weight.T, key_weight.T, value_weight.T, gate_weight.T], axis=0
    )
    neighbours = [(2 * y, 2 * (y ^ 1)) for y in range(8)]
    neighbours += [(2 * y + 1, 2 * (y + (1 if y % 2 else 7)) % 16 + 1) for y in range(8)]
    w_near = lax.ppermute(w_own, ("y", "tp"), neighbours)
    w_pair = moved(w_own, "tp", lambda i: i ^ 1)
    w_far = moved(w_near, "tp", lambda i: i ^ 1)

    o_own = out_weight.T
    ahead = [(2 * i, 2 * ((i + 1) % 4)) for i in range(4)]
    ahead += [(2 * i + 1, 2 * ((i - 1) % 4) + 1) for i in range(4)]
    behind = [(target, source) for source, target in ahead]

    def turned_by(value, pairs):
        return lax.ppermute(value, ("far_z", "tp"), pairs)

    turn_a = turned_by(o_own, ahead)
    turn_b = turned_by(o_own, behind)
    turn_c = turned_by(turn_a, ahead)
    out_blocks = [o_own, turn_a, turn_b, turn_c]

    log_decay = -decay_rate
    taken_state = next_state(prior_state, last_keys, last_values, accepted, log_decay)

    place = jnp.stack([core, y_index & 1]).astype(jnp.int32)
    weights, gain = arrange(
        place, norm_gain.reshape(-1, owned_seqs), (w_own, w_near, w_pair, w_far)
    )
    columns = project(arrived.reshape(width, owned_seqs), gain, weights)
    span = columns.shape[-1]
    columns = scattered(columns.reshape(128, local_seqs, span), KV_TP)
    pieces = columns.reshape(8, 4, 2, 2, local_seqs, span)
    lane = jnp.arange(span)
    unit = span // 12
    even_part = jnp.where(lane < 4 * unit, (lane // unit) % 2, (lane // (2 * unit)) % 2) == 0
    odd_source = (jnp.arange(2) == 1)[:, None, None, None]
    shifted = (core == 1) & (odd_source == even_part)
    turned_pieces = jnp.where(
        odd_source, jnp.roll(pieces, 1, axis=1), jnp.roll(pieces, -1, axis=1)
    )
    pieces = jnp.where(shifted, turned_pieces, pieces)

    def role_rows(first, last, size):
        picked = pieces[..., first:last].transpose(4, 3, 2, 0, 1, 5)
        return picked.reshape(local_seqs, proposals, heads_here, size)

    sixth = span // 6
    query_rows = role_rows(0, sixth, key_size)
    key_rows = role_rows(sixth, 2 * sixth, key_size)
    value_rows = role_rows(2 * sixth, 4 * sixth, value_size)
    gate_rows = role_rows(4 * sixth, 6 * sixth, value_size)
    positions = (lengths + accepted)[:, None] + jnp.arange(proposals, dtype=jnp.int32)[None, :]
    query_rot = rotate(query_rows, positions).astype(HALF)
    key_rot = (rotate(key_rows, positions) * key_size ** (-0.5)).astype(HALF)
    heads_out = retain(query_rot, key_rot, value_rows, taken_state, log_decay)
    head_norm = heads_out * lax.rsqrt(
        jnp.mean(heads_out * heads_out, axis=-1, keepdims=True) + epsilon
    )
    gated = (jax.nn.silu(gate_rows.astype(FLOAT)) * head_norm).astype(HALF)
    depth = heads_here * value_size
    gated = gated.reshape(1, local_seqs * proposals, depth)
    gated = jnp.broadcast_to(gated, (16, local_seqs * proposals, depth))
    gathered = scattered(gated, ("near_z", "y"))
    far_place = jnp.stack([far_index, core]).astype(jnp.int32)
    partial_out = output_product(
        far_place, gathered.reshape(16 * local_seqs * proposals, depth), out_blocks
    )
    terms = scattered(partial_out, ("far_z", "tp"))
    terms = terms.reshape(4, 2, *terms.shape[1:]).astype(FLOAT)
    retained = (terms[:, 0] + terms[:, 1]).astype(HALF)
    retained = retained.reshape(owned_seqs, proposals, -1)
    return (retained, taken_state, key_rot, value_rows)


def solution(mesh):
    finer = Mesh(
        mesh.devices.reshape(mesh.shape["dp"], 4, 2, 8, mesh.shape["tp"]), ("dp", *KV, "tp")
    )
    return jax.shard_map(
        shards,
        mesh=finer,
        in_specs=(
            P("dp", None, KV),
            P(),
            P(None, TP_KV),
            P(None, TP_KV),
            P(None, TP_KV),
            P(None, TP_KV),
            P("tp", KV),
            P("tp"),
            P(DP_KV, "tp", None, None),
            P(DP_KV, None, "tp", None),
            P(DP_KV, None, "tp", None),
            P(DP_KV),
            P(DP_KV),
        ),
        out_specs=(
            P("dp", None, KV_TP),
            P(DP_KV, "tp", None, None),
            P(DP_KV, None, "tp", None),
            P(DP_KV, None, "tp", None),
        ),
        check_vma=False,
    )
```

```python
import jax
import jax.numpy as jnp
from jax import lax
from jax.experimental import pallas as pl
from jax.experimental.pallas import tpu as pltpu
from jax.sharding import Mesh
from jax.sharding import PartitionSpec as P


KV = ("far_z", "near_z", "y")
TP_KV = ("tp", *KV)
DP_KV = ("dp", *KV)
KV_TP = (*KV, "tp")


epsilon = 1e-06
FLOAT = jnp.float32
HALF = jnp.bfloat16


def moved(value, axis, target):
    size = lax.axis_size(axis)
    return lax.ppermute(value, axis, [(i, target(i) % size) for i in range(size)])


def scattered(blocks, axes):
    return lax.all_to_all(blocks, axes, 0, 0, tiled=True)


def near(value):
    return pltpu.with_memory_space_constraint(value, pltpu.VMEM)


def rotate(field_in, positions):
    half_size = field_in.shape[-1] // 2
    frequency = jnp.power(10000.0, -jnp.arange(half_size, dtype=FLOAT) / half_size)
    angles = positions.astype(FLOAT)[:, :, None, None] * frequency
    cosine, sine_part = (jnp.cos(angles), jnp.sin(angles))
    floats = field_in.astype(FLOAT)
    first_half, second = (floats[..., :half_size], floats[..., half_size:])
    return jnp.concatenate(
        [first_half * cosine - second * sine_part, first_half * sine_part + second * cosine],
        axis=-1,
    )


def next_state(prior_state, last_keys, last_values, accepted, log_decay):
    highest = lax.Precision.HIGHEST
    step_ids = jnp.arange(last_keys.shape[1], dtype=jnp.int32)
    taken_mask = step_ids[None, :] < accepted[:, None]
    power_exp = jnp.maximum(accepted[:, None] - 1 - step_ids[None, :], 0).astype(FLOAT)
    weight = jnp.where(
        taken_mask[:, :, None], jnp.exp(log_decay[None, None, :] * power_exp[:, :, None]), 0.0
    )
    carried = jnp.exp(log_decay[None, :] * accepted[:, None].astype(FLOAT))
    weighted_keys = last_keys.astype(FLOAT) * weight[..., None]
    return carried[:, :, None, None] * prior_state + jnp.einsum(
        "sphd,sphe->shde", weighted_keys, last_values.astype(FLOAT), precision=highest
    )


def retain(query_rot, key_rot, value_rows, taken_state, log_decay):
    highest = lax.Precision.HIGHEST
    step_ids = jnp.arange(query_rot.shape[1], dtype=jnp.int32)
    scores = jnp.einsum(
        "sthd,smhd->shtm", query_rot.astype(FLOAT), key_rot.astype(FLOAT), precision=highest
    )
    offset = (step_ids[:, None] - step_ids[None, :]).astype(FLOAT)
    decay_grid = jnp.where(
        offset[None] >= 0.0, jnp.exp(log_decay[:, None, None] * jnp.maximum(offset, 0.0)[None]), 0.0
    )
    inner_sum = jnp.einsum(
        "shtm,smhe->sthe", scores * decay_grid[None], value_rows.astype(FLOAT), precision=highest
    )
    query_decay = jnp.exp(log_decay[None, :] * (step_ids[:, None].astype(FLOAT) + 1.0))
    cross_sum = jnp.einsum(
        "sthd,shde->sthe",
        query_rot.astype(FLOAT) * query_decay[None, :, :, None],
        taken_state,
        precision=lax.Precision.HIGH,
    )
    return inner_sum + cross_sum


def arrange_kernel(place, gain, w_own, w_near, w_pair, w_far, weights, columns):
    core, parity = place[0], place[1]
    key_cols = w_own.shape[0] // 6
    span = 2 * w_own.shape[0]
    for source, same_core, same_row in (
        (w_own, True, True),
        (w_near, True, False),
        (w_pair, False, True),
        (w_far, False, False),
    ):
        head_group = core if same_core else 1 - core
        later = parity if same_row else 1 - parity
        first = 0
        for size in (key_cols, key_cols, 2 * key_cols, 2 * key_cols):
            start = pl.multiple_of(head_group * span + 2 * first + later * size, 16)
            weights[pl.ds(start, size), :] = source[first : first + size, :]
            first += size
    side = gain.shape[1]
    floats = gain[...].astype(FLOAT)
    for row in range(gain.shape[0]):
        square = jnp.broadcast_to(floats[row : row + 1], (side, side)).T
        columns[row * side : (row + 1) * side, :] = square.astype(HALF)


def arrange(place, gain, sources):
    cols, width = sources[0].shape
    vmem = pl.BlockSpec(memory_space=pltpu.VMEM)
    side = gain.shape[1]
    return pl.pallas_call(
        arrange_kernel,
        in_specs=[pl.BlockSpec(memory_space=pltpu.SMEM)] + [vmem] * 5,
        out_specs=(vmem, vmem),
        out_shape=(
            pltpu.HBM((4 * cols, width), HALF),
            pltpu.VMEM((width, side), HALF),
        ),
        name="arrange",
        compiler_params=pltpu.CompilerParams(vmem_limit_bytes=16 << 20),
    )(place, gain, *sources)


def project_kernel(rows, gain, far_weights, out, weights, arrival):
    fetch = pltpu.make_async_copy(far_weights, weights, arrival)
    fetch.start()
    width = rows.shape[0]
    span = weights.shape[0] // 2
    floats = rows[...].astype(FLOAT)
    squares = jnp.sum(floats * floats, axis=0, keepdims=True)
    row_scale = lax.rsqrt(squares / width + epsilon)
    normed = (floats * row_scale * gain[...].astype(FLOAT)).astype(HALF)
    fetch.wait()
    product = jnp.dot(weights[...], normed, preferred_element_type=FLOAT)
    seqs = out.shape[2]
    for head_group in range(2):
        part = product[head_group * span : (head_group + 1) * span].T
        out[:, head_group] = part.reshape(-1, seqs, span).astype(HALF)


def project(rows, gain, weights):
    vmem = pl.BlockSpec(memory_space=pltpu.VMEM)
    return pl.pallas_call(
        project_kernel,
        in_specs=[vmem, vmem, pl.BlockSpec(memory_space=pltpu.HBM)],
        out_specs=vmem,
        out_shape=pltpu.VMEM((64, 2, 2, weights.shape[0] // 2), HALF),
        scratch_shapes=[pltpu.VMEM(weights.shape, HALF), pltpu.SemaphoreType.DMA],
        name="project",
        compiler_params=pltpu.CompilerParams(vmem_limit_bytes=24 << 20),
    )(near(rows), near(gain), pltpu.with_memory_space_constraint(weights, pltpu.HBM))


def output_kernel(place, rows, *refs):
    blocks, out, weights, product = refs[:-3], refs[-3], refs[-2], refs[-1]
    here, ring = place[0], 4
    cols = blocks[0].shape[0]
    quarter = cols // 2
    stride = 2 * place[1] - 1
    for turn, block in zip((0, stride, -stride, 2), blocks):
        start = pl.multiple_of(lax.rem(here + ring + turn, ring) * cols, cols)
        weights[pl.ds(start, cols), :] = block[...]
    total = lax.dot_general(
        rows[...], weights[...], (((1,), (1,)), ((), ())), preferred_element_type=FLOAT
    )
    groups, row_count, lanes = product.shape
    for group in range(groups):
        product[group] = total[:, group * lanes : (group + 1) * lanes]
    proposals = 4
    seqs = row_count // proposals
    for group in range(groups):
        parts = [product[group, pl.ds(p, seqs, stride=proposals), :] for p in range(proposals)]
        for block in range(lanes // quarter):
            pieces = [part[:, block * quarter : (block + 1) * quarter] for part in parts]
            joined = jnp.concatenate(pieces, axis=1)
            out[group * (lanes // quarter) + block] = joined.astype(HALF)


def output_product(place, rows, blocks):
    vmem = pl.BlockSpec(memory_space=pltpu.VMEM)
    cols, depth = blocks[0].shape
    quarter = cols // 2
    row_count = rows.shape[0]
    return pl.pallas_call(
        output_kernel,
        in_specs=[pl.BlockSpec(memory_space=pltpu.SMEM)] + [vmem] * (1 + len(blocks)),
        out_specs=vmem,
        out_shape=pltpu.VMEM((8, row_count // 4, 4 * quarter), HALF),
        scratch_shapes=[
            pltpu.VMEM((4 * cols, depth), HALF),
            pltpu.VMEM((4 * cols // 128, row_count, 128), FLOAT),
        ],
        name="output",
        compiler_params=pltpu.CompilerParams(vmem_limit_bytes=16 << 20),
    )(place, near(rows), *blocks)


def shards(
    tokens,
    norm_gain,
    query_weight,
    key_weight,
    value_weight,
    gate_weight,
    out_weight,
    decay_rate,
    prior_state,
    last_keys,
    last_values,
    accepted,
    lengths,
):
    owned_seqs, proposals, own_width = tokens.shape
    local_seqs, heads_here, key_size, value_size = prior_state.shape
    width = norm_gain.shape[0]
    core = lax.axis_index("tp")
    y_index = lax.axis_index("y")
    far_index = lax.axis_index("far_z")

    turned = tokens.transpose(1, 2, 0)
    mine = lax.dynamic_slice_in_dim(turned, 2 * core, 2, 0)
    copies = jnp.broadcast_to(mine[None], (32, 2, own_width, owned_seqs))
    copies = copies.reshape(64, own_width, owned_seqs)
    arrived = scattered(copies, KV)

    w_own = jnp.concatenate(
        [query_weight.T, key_weight.T, value_weight.T, gate_weight.T], axis=0
    )
    neighbours = [(2 * y, 2 * (y ^ 1)) for y in range(8)]
    neighbours += [(2 * y + 1, 2 * (y + (1 if y % 2 else 7)) % 16 + 1) for y in range(8)]
    w_near = lax.ppermute(w_own, ("y", "tp"), neighbours)
    w_pair = moved(w_own, "tp", lambda i: i ^ 1)
    w_far = moved(w_near, "tp", lambda i: i ^ 1)

    o_own = out_weight.T
    ahead = [(2 * i, 2 * ((i + 1) % 4)) for i in range(4)]
    ahead += [(2 * i + 1, 2 * ((i - 1) % 4) + 1) for i in range(4)]
    behind = [(target, source) for source, target in ahead]

    def turned_by(value, pairs):
        return lax.ppermute(value, ("far_z", "tp"), pairs)

    turn_a = turned_by(o_own, ahead)
    turn_b = turned_by(o_own, behind)
    turn_c = turned_by(turn_a, ahead)
    out_blocks = [o_own, turn_a, turn_b, turn_c]

    log_decay = -decay_rate
    taken_state = next_state(prior_state, last_keys, last_values, accepted, log_decay)

    place = jnp.stack([core, y_index & 1]).astype(jnp.int32)
    weights, gain = arrange(
        place, norm_gain.reshape(-1, owned_seqs), (w_own, w_near, w_pair, w_far)
    )
    columns = project(arrived.reshape(width, owned_seqs), gain, weights)
    span = columns.shape[-1]
    columns = scattered(columns.reshape(128, local_seqs, span), KV_TP)
    pieces = columns.reshape(8, 4, 2, 2, local_seqs, span)
    lane = jnp.arange(span)
    unit = span // 12
    even_part = jnp.where(lane < 4 * unit, (lane // unit) % 2, (lane // (2 * unit)) % 2) == 0
    odd_source = (jnp.arange(2) == 1)[:, None, None, None]
    shifted = (core == 1) & (odd_source == even_part)
    turned_pieces = jnp.where(
        odd_source, jnp.roll(pieces, 1, axis=1), jnp.roll(pieces, -1, axis=1)
    )
    pieces = jnp.where(shifted, turned_pieces, pieces)

    def role_rows(first, last, size, source=pieces):
        picked = source[..., first:last].transpose(4, 3, 2, 0, 1, 5)
        return picked.reshape(local_seqs, proposals, heads_here, size)

    sixth = span // 6
    query_rows = role_rows(0, sixth, key_size)
    key_rows = role_rows(sixth, 2 * sixth, key_size)
    value_rows = role_rows(2 * sixth, 4 * sixth, value_size)
    gate_rows = role_rows(4 * sixth, 6 * sixth, value_size)
    positions = (lengths + accepted)[:, None] + jnp.arange(proposals, dtype=jnp.int32)[None, :]
    query_rot = rotate(query_rows, positions).astype(HALF)
    key_rot = (rotate(key_rows, positions) * key_size ** (-0.5)).astype(HALF)
    heads_out = retain(query_rot, key_rot, value_rows, taken_state, log_decay)
    head_norm = heads_out * lax.rsqrt(
        jnp.mean(heads_out * heads_out, axis=-1, keepdims=True) + epsilon
    )
    gated = (jax.nn.silu(gate_rows.astype(FLOAT)) * head_norm).astype(HALF)
    depth = heads_here * value_size
    gated = gated.reshape(1, local_seqs * proposals, depth)
    gated = jnp.broadcast_to(gated, (16, local_seqs * proposals, depth))
    gathered = scattered(gated, ("near_z", "y"))
    late_pieces, gathered = lax.optimization_barrier((pieces, gathered))
    far_place = jnp.stack([far_index, core]).astype(jnp.int32)
    partial_out = output_product(
        far_place, gathered.reshape(16 * local_seqs * proposals, depth), out_blocks
    )
    terms = scattered(partial_out, ("far_z", "tp"))
    new_values = role_rows(2 * sixth, 4 * sixth, value_size, late_pieces)
    terms = terms.reshape(4, 2, *terms.shape[1:]).astype(FLOAT)
    retained = (terms[:, 0] + terms[:, 1]).astype(HALF)
    retained = retained.reshape(owned_seqs, proposals, -1)
    return (retained, taken_state, key_rot, new_values)


def solution(mesh):
    finer = Mesh(
        mesh.devices.reshape(mesh.shape["dp"], 4, 2, 8, mesh.shape["tp"]), ("dp", *KV, "tp")
    )
    return jax.shard_map(
        shards,
        mesh=finer,
        in_specs=(
            P("dp", None, KV),
            P(),
            P(None, TP_KV),
            P(None, TP_KV),
            P(None, TP_KV),
            P(None, TP_KV),
            P("tp", KV),
            P("tp"),
            P(DP_KV, "tp", None, None),
            P(DP_KV, None, "tp", None),
            P(DP_KV, None, "tp", None),
            P(DP_KV),
            P(DP_KV),
        ),
        out_specs=(
            P("dp", None, KV_TP),
            P(DP_KV, "tp", None, None),
            P(DP_KV, None, "tp", None),
            P(DP_KV, None, "tp", None),
        ),
        check_vma=False,
    )
```

```python
import jax
import jax.numpy as jnp
from jax import lax
from jax.experimental import pallas as pl
from jax.experimental.pallas import tpu as pltpu
from jax.sharding import Mesh
from jax.sharding import PartitionSpec as P


KV = ("far_z", "near_z", "y")
TP_KV = ("tp", *KV)
DP_KV = ("dp", *KV)
KV_TP = (*KV, "tp")


epsilon = 1e-06
FLOAT = jnp.float32
HALF = jnp.bfloat16


def moved(value, axis, target):
    size = lax.axis_size(axis)
    return lax.ppermute(value, axis, [(i, target(i) % size) for i in range(size)])


def scattered(blocks, axes):
    return lax.all_to_all(blocks, axes, 0, 0, tiled=True)


def near(value):
    return pltpu.with_memory_space_constraint(value, pltpu.VMEM)


def rotate(field_in, positions):
    half_size = field_in.shape[-1] // 2
    frequency = jnp.power(10000.0, -jnp.arange(half_size, dtype=FLOAT) / half_size)
    angles = positions.astype(FLOAT)[:, :, None, None] * frequency
    cosine, sine_part = (jnp.cos(angles), jnp.sin(angles))
    floats = field_in.astype(FLOAT)
    first_half, second = (floats[..., :half_size], floats[..., half_size:])
    return jnp.concatenate(
        [first_half * cosine - second * sine_part, first_half * sine_part + second * cosine],
        axis=-1,
    )


def next_state(prior_state, last_keys, last_values, accepted, log_decay):
    highest = lax.Precision.HIGHEST
    step_ids = jnp.arange(last_keys.shape[1], dtype=jnp.int32)
    taken_mask = step_ids[None, :] < accepted[:, None]
    power_exp = jnp.maximum(accepted[:, None] - 1 - step_ids[None, :], 0).astype(FLOAT)
    weight = jnp.where(
        taken_mask[:, :, None], jnp.exp(log_decay[None, None, :] * power_exp[:, :, None]), 0.0
    )
    carried = jnp.exp(log_decay[None, :] * accepted[:, None].astype(FLOAT))
    weighted_keys = last_keys.astype(FLOAT) * weight[..., None]
    return carried[:, :, None, None] * prior_state + jnp.einsum(
        "sphd,sphe->shde", weighted_keys, last_values.astype(FLOAT), precision=highest
    )


def retain(query_rot, key_rot, value_rows, taken_state, log_decay):
    step_ids = jnp.arange(query_rot.shape[1], dtype=jnp.int32)
    scores = jnp.einsum(
        "sthd,smhd->shtm", query_rot, key_rot, preferred_element_type=FLOAT
    )
    offset = (step_ids[:, None] - step_ids[None, :]).astype(FLOAT)
    decay_grid = jnp.where(
        offset[None] >= 0.0, jnp.exp(log_decay[:, None, None] * jnp.maximum(offset, 0.0)[None]), 0.0
    )
    inner_sum = jnp.einsum(
        "shtm,smhe->sthe", scores * decay_grid[None], value_rows.astype(FLOAT), precision=lax.Precision.HIGH
    )
    query_decay = jnp.exp(log_decay[None, :] * (step_ids[:, None].astype(FLOAT) + 1.0))
    cross_sum = jnp.einsum(
        "sthd,shde->sthe",
        query_rot.astype(FLOAT) * query_decay[None, :, :, None],
        taken_state,
        precision=lax.Precision.HIGH,
    )
    return inner_sum + cross_sum


def arrange_kernel(place, gain, w_own, w_near, w_pair, w_far, weights, columns):
    core, parity = place[0], place[1]
    key_cols = w_own.shape[0] // 6
    span = 2 * w_own.shape[0]
    for source, same_core, same_row in (
        (w_own, True, True),
        (w_near, True, False),
        (w_pair, False, True),
        (w_far, False, False),
    ):
        head_group = core if same_core else 1 - core
        later = parity if same_row else 1 - parity
        first = 0
        for size in (key_cols, key_cols, 2 * key_cols, 2 * key_cols):
            start = pl.multiple_of(head_group * span + 2 * first + later * size, 16)
            weights[pl.ds(start, size), :] = source[first : first + size, :]
            first += size
    side = gain.shape[1]
    floats = gain[...].astype(FLOAT)
    for row in range(gain.shape[0]):
        square = jnp.broadcast_to(floats[row : row + 1], (side, side)).T
        columns[row * side : (row + 1) * side, :] = square.astype(HALF)


def arrange(place, gain, sources):
    cols, width = sources[0].shape
    vmem = pl.BlockSpec(memory_space=pltpu.VMEM)
    side = gain.shape[1]
    return pl.pallas_call(
        arrange_kernel,
        in_specs=[pl.BlockSpec(memory_space=pltpu.SMEM)] + [vmem] * 5,
        out_specs=(vmem, vmem),
        out_shape=(
            pltpu.HBM((4 * cols, width), HALF),
            pltpu.VMEM((width, side), HALF),
        ),
        name="arrange",
        compiler_params=pltpu.CompilerParams(vmem_limit_bytes=16 << 20),
    )(place, gain, *sources)


def project_kernel(rows, gain, far_weights, out, weights, arrival):
    fetch = pltpu.make_async_copy(far_weights, weights, arrival)
    fetch.start()
    width = rows.shape[0]
    span = weights.shape[0] // 2
    floats = rows[...].astype(FLOAT)
    squares = jnp.sum(floats * floats, axis=0, keepdims=True)
    row_scale = lax.rsqrt(squares / width + epsilon)
    normed = (floats * row_scale * gain[...].astype(FLOAT)).astype(HALF)
    fetch.wait()
    product = jnp.dot(weights[...], normed, preferred_element_type=FLOAT)
    seqs = out.shape[2]
    for head_group in range(2):
        part = product[head_group * span : (head_group + 1) * span].T
        out[:, head_group] = part.reshape(-1, seqs, span).astype(HALF)


def project(rows, gain, weights):
    vmem = pl.BlockSpec(memory_space=pltpu.VMEM)
    return pl.pallas_call(
        project_kernel,
        in_specs=[vmem, vmem, pl.BlockSpec(memory_space=pltpu.HBM)],
        out_specs=vmem,
        out_shape=pltpu.VMEM((64, 2, 2, weights.shape[0] // 2), HALF),
        scratch_shapes=[pltpu.VMEM(weights.shape, HALF), pltpu.SemaphoreType.DMA],
        name="project",
        compiler_params=pltpu.CompilerParams(vmem_limit_bytes=24 << 20),
    )(near(rows), near(gain), pltpu.with_memory_space_constraint(weights, pltpu.HBM))


def output_kernel(place, rows, *refs):
    blocks, out, weights, product = refs[:-3], refs[-3], refs[-2], refs[-1]
    here, ring = place[0], 4
    cols = blocks[0].shape[0]
    quarter = cols // 2
    stride = 2 * place[1] - 1
    for turn, block in zip((0, stride, -stride, 2), blocks):
        start = pl.multiple_of(lax.rem(here + ring + turn, ring) * cols, cols)
        weights[pl.ds(start, cols), :] = block[...]
    total = lax.dot_general(
        rows[...], weights[...], (((1,), (1,)), ((), ())), preferred_element_type=FLOAT
    )
    groups, row_count, lanes = product.shape
    for group in range(groups):
        product[group] = total[:, group * lanes : (group + 1) * lanes]
    proposals = 4
    seqs = row_count // proposals
    for group in range(groups):
        parts = [product[group, pl.ds(p, seqs, stride=proposals), :] for p in range(proposals)]
        for block in range(lanes // quarter):
            pieces = [part[:, block * quarter : (block + 1) * quarter] for part in parts]
            joined = jnp.concatenate(pieces, axis=1)
            out[group * (lanes // quarter) + block] = joined.astype(HALF)


def output_product(place, rows, blocks):
    vmem = pl.BlockSpec(memory_space=pltpu.VMEM)
    cols, depth = blocks[0].shape
    quarter = cols // 2
    row_count = rows.shape[0]
    return pl.pallas_call(
        output_kernel,
        in_specs=[pl.BlockSpec(memory_space=pltpu.SMEM)] + [vmem] * (1 + len(blocks)),
        out_specs=vmem,
        out_shape=pltpu.VMEM((8, row_count // 4, 4 * quarter), HALF),
        scratch_shapes=[
            pltpu.VMEM((4 * cols, depth), HALF),
            pltpu.VMEM((4 * cols // 128, row_count, 128), FLOAT),
        ],
        name="output",
        compiler_params=pltpu.CompilerParams(vmem_limit_bytes=16 << 20),
    )(place, near(rows), *blocks)


def shards(
    tokens,
    norm_gain,
    query_weight,
    key_weight,
    value_weight,
    gate_weight,
    out_weight,
    decay_rate,
    prior_state,
    last_keys,
    last_values,
    accepted,
    lengths,
):
    owned_seqs, proposals, own_width = tokens.shape
    local_seqs, heads_here, key_size, value_size = prior_state.shape
    width = norm_gain.shape[0]
    core = lax.axis_index("tp")
    y_index = lax.axis_index("y")
    far_index = lax.axis_index("far_z")

    turned = tokens.transpose(1, 2, 0)
    mine = lax.dynamic_slice_in_dim(turned, 2 * core, 2, 0)
    copies = jnp.broadcast_to(mine[None], (32, 2, own_width, owned_seqs))
    copies = copies.reshape(64, own_width, owned_seqs)
    arrived = scattered(copies, KV)

    w_own = jnp.concatenate(
        [query_weight.T, key_weight.T, value_weight.T, gate_weight.T], axis=0
    )
    neighbours = [(2 * y, 2 * (y ^ 1)) for y in range(8)]
    neighbours += [(2 * y + 1, 2 * (y + (1 if y % 2 else 7)) % 16 + 1) for y in range(8)]
    w_near = lax.ppermute(w_own, ("y", "tp"), neighbours)
    w_pair = moved(w_own, "tp", lambda i: i ^ 1)
    w_far = moved(w_near, "tp", lambda i: i ^ 1)

    o_own = out_weight.T
    ahead = [(2 * i, 2 * ((i + 1) % 4)) for i in range(4)]
    ahead += [(2 * i + 1, 2 * ((i - 1) % 4) + 1) for i in range(4)]
    behind = [(target, source) for source, target in ahead]

    def turned_by(value, pairs):
        return lax.ppermute(value, ("far_z", "tp"), pairs)

    turn_a = turned_by(o_own, ahead)
    turn_b = turned_by(o_own, behind)
    turn_c = turned_by(turn_a, ahead)
    out_blocks = [o_own, turn_a, turn_b, turn_c]

    log_decay = -decay_rate
    taken_state = next_state(prior_state, last_keys, last_values, accepted, log_decay)

    place = jnp.stack([core, y_index & 1]).astype(jnp.int32)
    weights, gain = arrange(
        place, norm_gain.reshape(-1, owned_seqs), (w_own, w_near, w_pair, w_far)
    )
    columns = project(arrived.reshape(width, owned_seqs), gain, weights)
    span = columns.shape[-1]
    columns = scattered(columns.reshape(128, local_seqs, span), KV_TP)
    pieces = columns.reshape(8, 4, 2, 2, local_seqs, span)
    lane = jnp.arange(span)
    unit = span // 12
    even_part = jnp.where(lane < 4 * unit, (lane // unit) % 2, (lane // (2 * unit)) % 2) == 0
    odd_source = (jnp.arange(2) == 1)[:, None, None, None]
    shifted = (core == 1) & (odd_source == even_part)
    turned_pieces = jnp.where(
        odd_source, jnp.roll(pieces, 1, axis=1), jnp.roll(pieces, -1, axis=1)
    )
    pieces = jnp.where(shifted, turned_pieces, pieces)

    def role_rows(first, last, size, source=pieces):
        picked = source[..., first:last].transpose(4, 3, 2, 0, 1, 5)
        return picked.reshape(local_seqs, proposals, heads_here, size)

    sixth = span // 6
    query_rows = role_rows(0, sixth, key_size)
    key_rows = role_rows(sixth, 2 * sixth, key_size)
    value_rows = role_rows(2 * sixth, 4 * sixth, value_size)
    gate_rows = role_rows(4 * sixth, 6 * sixth, value_size)
    positions = (lengths + accepted)[:, None] + jnp.arange(proposals, dtype=jnp.int32)[None, :]
    query_rot = rotate(query_rows, positions).astype(HALF)
    key_rot = (rotate(key_rows, positions) * key_size ** (-0.5)).astype(HALF)
    heads_out = retain(query_rot, key_rot, value_rows, taken_state, log_decay)
    head_norm = heads_out * lax.rsqrt(
        jnp.mean(heads_out * heads_out, axis=-1, keepdims=True) + epsilon
    )
    gated = (jax.nn.silu(gate_rows.astype(FLOAT)) * head_norm).astype(HALF)
    depth = heads_here * value_size
    gated = gated.reshape(1, local_seqs * proposals, depth)
    gated = jnp.broadcast_to(gated, (16, local_seqs * proposals, depth))
    gathered = scattered(gated, ("near_z", "y"))
    late_pieces, gathered = lax.optimization_barrier((pieces, gathered))
    far_place = jnp.stack([far_index, core]).astype(jnp.int32)
    partial_out = output_product(
        far_place, gathered.reshape(16 * local_seqs * proposals, depth), out_blocks
    )
    terms = scattered(partial_out, ("far_z", "tp"))
    new_values = role_rows(2 * sixth, 4 * sixth, value_size, late_pieces)
    terms = terms.reshape(4, 2, *terms.shape[1:]).astype(FLOAT)
    retained = (terms[:, 0] + terms[:, 1]).astype(HALF)
    retained = retained.reshape(owned_seqs, proposals, -1)
    return (retained, taken_state, key_rot, new_values)


def solution(mesh):
    finer = Mesh(
        mesh.devices.reshape(mesh.shape["dp"], 4, 2, 8, mesh.shape["tp"]), ("dp", *KV, "tp")
    )
    return jax.shard_map(
        shards,
        mesh=finer,
        in_specs=(
            P("dp", None, KV),
            P(),
            P(None, TP_KV),
            P(None, TP_KV),
            P(None, TP_KV),
            P(None, TP_KV),
            P("tp", KV),
            P("tp"),
            P(DP_KV, "tp", None, None),
            P(DP_KV, None, "tp", None),
            P(DP_KV, None, "tp", None),
            P(DP_KV),
            P(DP_KV),
        ),
        out_specs=(
            P("dp", None, KV_TP),
            P(DP_KV, "tp", None, None),
            P(DP_KV, None, "tp", None),
            P(DP_KV, None, "tp", None),
        ),
        check_vma=False,
    )
```
